256 devices in a mesh: grp: 2 (over y), fs: 16 (over z), tp: 8 (over x, core).
Axes of the slice: x: 4, y: 2, z: 16, core: 2. Of those that a mesh axis runs over, the one named last changes fastest.
The devices are a block of a 4x16x16 slice.
Arguments:
- tokens: bfloat16 [8192, 2048], P(('grp', 'fs')), parts along dimension 0, may hold values from -6 to 6
- route_ids: int32 [8192, 2], P(('grp', 'fs')), parts along dimension 0, may hold values from 0 to 31, as said below
- route_weights: float32 [8192, 2], P(('grp', 'fs')), parts along dimension 0, may hold values from 0.2 to 1
- ffn_gain: float32 [2048], P('fs'), may hold values from 0.1 to 1.9
- gate_master: float32 [32, 2048, 1024], P(None, 'fs', 'tp'), may hold values from -0.125 to 0.125
- up_master: float32 [32, 2048, 1024], P(None, 'fs', 'tp'), may hold values from -0.125 to 0.125
- down_master: float32 [32, 1024, 2048], P(None, 'fs', 'tp'), may hold values from -0.1875 to 0.1875
Outputs:
- gate_serve: bfloat16 [64, 2048, 1024], P(('grp', 'fs'), None, 'tp'), parts along dimension 0
- up_serve: bfloat16 [64, 2048, 1024], P(('grp', 'fs'), None, 'tp'), parts along dimension 0
- down_serve: bfloat16 [64, 1024, 2048], P(('grp', 'fs'), None, 'tp'), parts along dimension 0
- mixed: bfloat16 [8192, 2048], P(('grp', 'fs'), 'tp'), parts along dimension 0
The draws below stay inside these ranges and needn't reach their ends.
There are 2 independent parts, one for each index of `grp`. The reference program is written for one: setup_inputs(seed, part) draws one part's arguments, and reference() takes and returns one part's arrays. A program takes and returns all parts, laid end to end along the dimension named above; an argument that names none is the same for every part. Nothing has to cross between parts.
Inputs may be any that keep to these rules, and one draw needn't show every extreme that they name: `route_ids`: each row names two different experts of one group of 8 consecutive experts. Among the tokens of one index of fs, each group is named by exactly 64 tokens and no expert by more than 32; in every group one expert, the same for every index of fs, is named by exactly 32, and so is one other expert of the group, which may change from one index of fs to the next.
All inputs are finite; a program needn't handle non-finite values.
Results may differ from the reference program's by a relative error of at most 0.0087.
Values may be sent and summed in bfloat16 or wider, within the bound.
A program may use at most 64 MiB of HBM per device.

```python
import jax
import jax.numpy as jnp
from jax import lax

D = 2048
FF = 1024
GROUP_SIZE = 8
TOK_DEV = 256
EXPERTS = 32
GROUPS = 4
CAP = 32
TOKENS = 4096
N_FS = 16


def draw_route_ids(key, part):
    blocks = TOKENS // TOK_DEV
    per_group = TOK_DEV // GROUPS
    half_group = per_group // 2
    others_count = GROUP_SIZE - 2
    hot_local = jax.random.randint(jax.random.fold_in(key, 11), (GROUPS,), 0, GROUP_SIZE).astype(jnp.int32)
    rank_list = jnp.arange(TOK_DEV, dtype=jnp.int32)
    group_of = rank_list // per_group
    within = rank_list % per_group
    leading = within < half_group
    local_list = jnp.arange(GROUP_SIZE, dtype=jnp.int32)
    block_keys = jax.random.split(jax.random.fold_in(key, 13), blocks)
    block_list = jnp.arange(blocks, dtype=jnp.int32)

    def one_block(subkey, block_index):
        step_draw = jax.random.randint(jax.random.fold_in(subkey, 4), (GROUPS,), 0, GROUP_SIZE - 1).astype(jnp.int32)
        drawn_second = (hot_local + 1 + step_draw) % GROUP_SIZE
        paired = jnp.bitwise_xor(hot_local, 1)
        second_full = jnp.where(block_index % 2 == 0, paired, drawn_second)
        group_keys = jax.random.split(jax.random.fold_in(subkey, 3), GROUPS)
        ranks = jax.vmap(lambda inner_key: jax.random.permutation(inner_key, GROUP_SIZE))(group_keys).astype(jnp.int32)
        excluded = (local_list[None, :] == hot_local[:, None]) | (local_list[None, :] == second_full[:, None])
        scores = ranks + GROUP_SIZE * excluded.astype(jnp.int32)
        ordered = jnp.argsort(scores, axis=1).astype(jnp.int32)
        others = ordered[:, :others_count]
        first_local = jnp.where(leading, hot_local[group_of], second_full[group_of])
        second_local = others[group_of, within % others_count]
        pairing = jnp.stack([first_local, second_local], axis=1) + group_of[:, None] * GROUP_SIZE
        placing = jax.random.permutation(jax.random.fold_in(subkey, 1), TOK_DEV)
        flipped = jax.random.randint(jax.random.fold_in(subkey, 2), (TOK_DEV, 1), 0, 2)
        swapped = jnp.where(flipped == 1, pairing[:, ::-1], pairing)
        return jnp.zeros((TOK_DEV, 2), jnp.int32).at[placing].set(swapped.astype(jnp.int32))
    return jax.vmap(one_block)(block_keys, block_list).reshape(TOKENS, 2).astype(jnp.int32)


def shard_levels(key, extent, cuts, low, largest):
    def one(axis_at, shards_of):
        heights = jax.random.uniform(jax.random.fold_in(jax.random.fold_in(key, 6), axis_at), (shards_of,), jnp.float32, low / len(cuts), largest / len(cuts))
        return jnp.repeat(jnp.exp(heights), extent[axis_at] // shards_of).reshape((-1,) + (1,) * (len(extent) - axis_at - 1))

    factor_of = one(*cuts[0])
    for cut in cuts[1:]:
        factor_of = factor_of * one(*cut)
    return factor_of


def normal_values(key, dims, scale, limit, cuts=(), held_as=jnp.bfloat16):
    entries = jax.random.normal(key, dims, jnp.float32) * scale
    if len(cuts) > 0:
        entries = shard_levels(key, dims, cuts, -0.22, 0.18) * entries
    return jnp.clip(entries, min=-limit, max=limit).astype(held_as)


def setup_inputs(seed: int = 0, part: int = 0) -> dict:
    key_list = jax.random.split(jax.random.key(seed), 8)
    part_splits = jax.random.split(jax.random.fold_in(key_list[7], part), 8)
    tokens = normal_values(part_splits[0], (TOKENS, D), 1.0, 6.0, ((0, 16),))
    route_ids = draw_route_ids(jax.random.fold_in(jax.random.fold_in(key_list[7], part), 71), part)
    route_weights = jnp.clip(0.2 + 0.8 * jax.random.uniform(part_splits[2], (TOKENS, 2), jnp.float32) ** shard_levels(part_splits[2], (TOKENS, 2), ((0, 16),), -0.2, 0.2), 0.2, 1.0)
    ffn_gain = jnp.clip(1.0 + 0.18 * jax.random.normal(key_list[3], (D,), jnp.float32), 0.1, 1.9)
    gate_master = normal_values(key_list[4], (EXPERTS, D, FF), D ** -0.5, 0.125, ((1, 16), (2, 8)), jnp.float32)
    up_master = normal_values(key_list[5], (EXPERTS, D, FF), D ** -0.5, 0.125, ((1, 16), (2, 8)), jnp.float32)
    down_master = normal_values(key_list[6], (EXPERTS, FF, D), FF ** -0.5, 0.1875, ((1, 16), (2, 8)), jnp.float32)
    return {"tokens": tokens, "route_ids": route_ids, "route_weights": route_weights, "ffn_gain": ffn_gain, "gate_master": gate_master, "up_master": up_master, "down_master": down_master}


def reference(tokens, route_ids, route_weights, ffn_gain, gate_master, up_master, down_master):
    row_gain = ffn_gain.astype(jnp.float32)[None, :, None]
    gate_serve = (gate_master * row_gain).astype(jnp.bfloat16)
    up_serve = (up_master * row_gain).astype(jnp.bfloat16)
    down_serve = down_master.astype(jnp.bfloat16)
    token_rows = tokens.astype(jnp.float32)
    normed = (token_rows * lax.rsqrt(lax.optimization_barrier(jnp.mean(token_rows * token_rows, axis=1, keepdims=True)) + 1e-06)).astype(jnp.bfloat16)
    flat_ids = route_ids.reshape(-1).astype(jnp.int32)
    flat_weights = route_weights.reshape(-1).astype(jnp.float32)
    slot_limit = N_FS * CAP

    def one_expert(inputs):
        expert, w_gate, w_up, w_down = inputs
        matches = flat_ids == expert
        chosen = jnp.nonzero(matches, size=slot_limit, fill_value=0)[0].astype(jnp.int32)
        live_count = jnp.sum(matches.astype(jnp.int32))
        is_live = jnp.arange(slot_limit, dtype=jnp.int32) < live_count
        picked = normed[chosen // 2]
        gate_val = jnp.dot(picked, w_gate, preferred_element_type=jnp.float32)
        up_val = jnp.dot(picked, w_up, preferred_element_type=jnp.float32)
        hidden = (jax.nn.silu(gate_val) * up_val).astype(jnp.bfloat16)
        route_out = jnp.dot(hidden, w_down, preferred_element_type=jnp.float32).astype(jnp.bfloat16)
        route_scale = jnp.where(is_live, flat_weights[chosen], jnp.zeros_like(flat_weights[chosen]))
        return (chosen // 2, route_out.astype(jnp.float32) * route_scale[:, None])
    expert_list = jnp.arange(gate_serve.shape[0], dtype=jnp.int32)
    owners, terms = lax.map(one_expert, (expert_list, gate_serve, up_serve, down_serve))
    combined = jnp.zeros(tokens.shape, jnp.float32).at[owners.reshape(-1)].add(terms.reshape(-1, tokens.shape[1]))
    return (gate_serve, up_serve, down_serve, combined.astype(jnp.bfloat16))
```

```python
import functools

import jax
import jax.numpy as jnp
from jax import lax
from jax.experimental import pallas as pl
from jax.experimental.pallas import tpu as pltpu
from jax.sharding import PartitionSpec as P

GROUP_SIZE = 8
MESH = pl.DeviceIdType.MESH
BF16 = jnp.bfloat16
F32 = jnp.float32


def remote(src, dst, send, recv, where):
    return pltpu.make_async_remote_copy(
        src_ref=src, dst_ref=dst, send_sem=send, recv_sem=recv, device_id=where, device_id_type=MESH
    )


def kernel(
    n_fs, n_tp, span,
    tok_ref, ids_ref, rw_ref, gain_ref, gm_ref, um_ref, dm_ref,
    og_out, ou_out, od_out, mix_ref,
    g_in, u_in, d_in, g_own, u_own, d_own,
    g_send, u_send, d_send, og, ou, od,
    s_buf, w_send, x_buf, w_recv, h_buf, w_rows, part, gathered, total, final,
    load_sem, out_sem, z_send, z_recv, y_send, y_recv, tz_send, tz_recv,
    xs_sem, xr_sem, hs_sem, hr_sem, ps_sem, pr_sem, fs_sem, fr_sem,
):
    grp, me, t = lax.axis_index("grp"), lax.axis_index("fs"), lax.axis_index("tp")
    q = lax.rem(grp, 2)
    other = 1 - q
    mate = grp + 1 - 2 * q
    right, left = lax.rem(t + 2, n_tp), lax.rem(t + n_tp - 2, n_tp)
    far = lax.rem(t + 4, n_tp)
    twin = t + 1 - 2 * lax.rem(t, 2)
    member = lax.rem(me, span)
    base = me - member
    toks = tok_ref.shape[0]
    cols = s_buf.shape[1]
    per = s_buf.shape[0] // (n_fs // span)
    quarter = per // span

    def turn(i):
        half = lax.div(i, 2)
        odd = lax.rem(i, 2)
        return half + 1 + odd * (n_fs - 2 * half - 2)

    barrier = pltpu.get_barrier_semaphore()

    def greet(i, c):
        pl.semaphore_signal(
            barrier, inc=1, device_id={"fs": lax.rem(me + i, n_fs)}, device_id_type=MESH
        )
        return c

    lax.fori_loop(1, n_fs, greet, 0)
    pl.semaphore_signal(barrier, inc=1, device_id={"grp": mate}, device_id_type=MESH)
    for peer in (right, left, twin):
        pl.semaphore_signal(barrier, inc=1, device_id={"tp": peer}, device_id_type=MESH)

    loads = [
        pltpu.make_async_copy(gm_ref.at[:, q], g_in, load_sem.at[0]),
        pltpu.make_async_copy(um_ref.at[:, q], u_in, load_sem.at[1]),
        pltpu.make_async_copy(dm_ref.at[:, q], d_in, load_sem.at[2]),
        pltpu.make_async_copy(gm_ref.at[me, other], g_own, load_sem.at[3]),
        pltpu.make_async_copy(um_ref.at[me, other], u_own, load_sem.at[4]),
        pltpu.make_async_copy(dm_ref.at[me, other], d_own, load_sem.at[5]),
    ]
    for load in loads:
        load.start()

    ids = ids_ref[...]
    group = lax.shift_right_logical(ids[:, 0:1], GROUP_SIZE.bit_length() - 1)
    lane = lax.broadcasted_iota(jnp.int32, (toks, 128), 1)
    group_hot = (group == lane).astype(F32)
    row = lax.broadcasted_iota(jnp.int32, (toks, toks), 0)
    col = lax.broadcasted_iota(jnp.int32, (toks, toks), 1)
    earlier = (col < row).astype(BF16)
    counts = jnp.dot(earlier, group_hot.astype(BF16), preferred_element_type=F32)
    rank = jnp.sum(counts * group_hot, axis=1, keepdims=True)
    target = group.astype(F32) * per + rank
    place = (target == col.astype(F32)).astype(BF16)
    tok = tok_ref[...].astype(F32)
    scale = lax.rsqrt(jnp.mean(tok * tok, axis=1, keepdims=True) + 1e-06)
    own = tok_ref[:, pl.ds(pl.multiple_of(t * cols, cols), cols)].astype(F32)
    normed = (own * scale).astype(BF16)
    s_buf[...] = lax.dot_general(
        place, normed, (((0,), (0,)), ((), ())), preferred_element_type=F32
    ).astype(BF16)
    rw = rw_ref[...]
    by_expert = jnp.where(ids[:, 0:1] == lane, rw[:, 0:1], 0.0) + jnp.where(
        ids[:, 1:2] == lane, rw[:, 1:2], 0.0
    )
    rank_hot = (rank == lane.astype(F32)).astype(F32)
    w_all = lax.dot_general(
        by_expert, rank_hot, (((0,), (0,)), ((), ())),
        preferred_element_type=F32, precision=lax.Precision.HIGHEST,
    )
    for j in range(n_fs):
        w_send[j] = w_all[2 * j : 2 * j + 2]

    pl.semaphore_wait(barrier, n_fs - 1 + 4)

    def rows_at(buf, s):
        half = x_buf.shape[2] // per
        return buf.at[t, lax.div(s, half), pl.ds(pl.multiple_of(lax.rem(s, half) * per, per), per)]

    def tok_copy(j, s):
        begin = pl.multiple_of(lax.div(j, span) * per, per)
        return remote(
            s_buf.at[pl.ds(begin, per)], rows_at(x_buf, s), tz_send.at[0, j], tz_recv.at[0, s], {"fs": j}
        )

    def w_copy(j, s):
        return remote(w_send.at[j], w_recv.at[s], tz_send.at[1, j], tz_recv.at[1, s], {"fs": j})

    def dispatch(i, c):
        j = lax.rem(me + turn(i), n_fs)
        tok_copy(j, me).start()
        w_copy(j, me).start()
        return c

    lax.fori_loop(0, n_fs - 1, dispatch, 0)

    gain = jnp.broadcast_to(gain_ref[...], g_own.shape)
    gate_rows, down_rows = g_own.shape[0], d_own.shape[0]

    def gate_at(buf, e, s):
        return buf.at[e, pl.ds(pl.multiple_of(s * gate_rows, gate_rows), gate_rows)]

    def down_at(buf, e, s):
        return buf.at[e, pl.ds(pl.multiple_of(s * down_rows, down_rows), down_rows)]

    def z_copy(a, j, s):
        src = (g_send, u_send, d_send)[a].at[j]
        dst = (gate_at(og, q, s), gate_at(ou, q, s), down_at(od, q, s))[a]
        return remote(src, dst, z_send.at[a, j], z_recv.at[a, s], {"fs": j})

    def y_copy(a, e, s):
        spot = (gate_at(og, e, s), gate_at(ou, e, s), down_at(od, e, s))[a]
        return remote(spot, spot, y_send.at[a, s], y_recv.at[a, s], {"grp": mate})

    loads[0].wait()
    loads[1].wait()

    def send_gate_up(i, c):
        j = lax.rem(me + turn(i), n_fs)
        g_send[j] = (g_in[j] * gain).astype(BF16)
        u_send[j] = (u_in[j] * gain).astype(BF16)
        z_copy(0, j, me).start()
        z_copy(1, j, me).start()
        return c

    lax.fori_loop(0, n_fs - 1, send_gate_up, 0)
    for load in loads[2:]:
        load.wait()
    gate_spot = pl.ds(pl.multiple_of(me * gate_rows, gate_rows), gate_rows)
    down_spot = pl.ds(pl.multiple_of(me * down_rows, down_rows), down_rows)
    og[q, gate_spot] = (g_in[me] * gain).astype(BF16)
    ou[q, gate_spot] = (u_in[me] * gain).astype(BF16)
    od[q, down_spot] = d_in[me].astype(BF16)
    og[other, gate_spot] = (g_own[...] * gain).astype(BF16)
    ou[other, gate_spot] = (u_own[...] * gain).astype(BF16)
    od[other, down_spot] = d_own[...].astype(BF16)

    def send_down(i, c):
        j = lax.rem(me + turn(i), n_fs)
        d_send[j] = d_in[j].astype(BF16)
        z_copy(2, j, me).start()
        return c

    lax.fori_loop(0, n_fs - 1, send_down, 0)

    own_rows = s_buf[pl.ds(pl.multiple_of(lax.div(me, span) * per, per), per)]
    x_half = x_buf.shape[2] // per
    x_buf[t, lax.div(me, x_half), pl.ds(pl.multiple_of(lax.rem(me, x_half) * per, per), per)] = own_rows
    w_recv[me] = w_send[me]

    def tokens_in(i, c):
        s = lax.rem(me + n_fs - turn(i), n_fs)
        tok_copy(s, s).wait_recv()
        w_copy(s, s).wait_recv()
        return c

    lax.fori_loop(0, n_fs - 1, tokens_in, 0)

    def tp_gather(buf, send, recv):
        def to(block, k, peer):
            return remote(block, block, send.at[k], recv.at[k], {"tp": peer})

        first = [to(buf.at[t], 0, right), to(buf.at[t], 1, left), to(buf.at[t], 4, twin)]
        for copy in first:
            copy.start()
        to(buf.at[left], 0, right).wait_recv()
        second = [to(buf.at[left, 0], 2, right), to(buf.at[left], 5, twin)]
        for copy in second:
            copy.start()
        to(buf.at[right], 1, left).wait_recv()
        third = [to(buf.at[right, 1], 3, left), to(buf.at[right], 6, twin)]
        for copy in third:
            copy.start()
        to(buf.at[far, 0], 2, right).wait_recv()
        to(buf.at[far, 1], 3, left).wait_recv()
        fourth = [to(buf.at[far], 7, twin)]
        fourth[0].start()
        for k, shift in ((4, 0), (5, n_tp - 2), (6, 2), (7, 4)):
            to(buf.at[lax.rem(twin + shift, n_tp)], k, twin).wait_recv()
        return first + second + third + fourth

    sent = tp_gather(x_buf, xs_sem, xr_sem)

    def pass_gate_up(i, c):
        s = lax.rem(me + n_fs - turn(i), n_fs)
        for a in (0, 1):
            z_copy(a, s, s).wait_recv()
            y_copy(a, q, s).start()
        return c

    lax.fori_loop(0, n_fs - 1, pass_gate_up, 0)

    def mate_gate_up(i, c):
        s = lax.rem(me + n_fs - turn(i), n_fs)
        for a in (0, 1):
            y_copy(a, other, s).wait_recv()
        return c

    lax.fori_loop(0, n_fs - 1, mate_gate_up, 0)
    outs = [
        pltpu.make_async_copy(og, og_out, out_sem.at[0]),
        pltpu.make_async_copy(ou, ou_out, out_sem.at[1]),
        pltpu.make_async_copy(od, od_out, out_sem.at[2]),
    ]
    outs[0].start()
    outs[1].start()

    width = og.shape[2]
    tile = x_buf.shape[2]

    def hidden(i, c):
        half, k = lax.div(i, 2), lax.rem(i, 2)
        acc = jnp.zeros((tile, 2 * width), F32)
        for f in range(n_tp):
            w = jnp.concatenate(
                [og[k, f * cols : (f + 1) * cols], ou[k, f * cols : (f + 1) * cols]], axis=1
            )
            acc += jnp.dot(x_buf[f, half], w, preferred_element_type=F32)
        g, u = acc[:, :width], acc[:, width:]
        act = g / (1.0 + jnp.exp(-g)) * u
        h_buf[t, k, pl.ds(pl.multiple_of(half * tile, tile), tile)] = act.astype(BF16)
        return c

    lax.fori_loop(0, 4, hidden, 0)

    eye = (
        lax.broadcasted_iota(jnp.int32, (per, 128), 0) == lax.broadcasted_iota(jnp.int32, (per, 128), 1)
    ).astype(F32)

    def columns(s, c):
        both = w_recv[s]
        for k in range(2):
            column = jnp.sum(eye * both[k : k + 1], axis=1, keepdims=True)
            w_rows[k, pl.ds(pl.multiple_of(s * per, per), per)] = jnp.broadcast_to(column, (per, 128))
        return c

    lax.fori_loop(0, n_fs, columns, 0)

    sent += tp_gather(h_buf, hs_sem, hr_sem)

    def pass_down(i, c):
        s = lax.rem(me + n_fs - turn(i), n_fs)
        z_copy(2, s, s).wait_recv()
        y_copy(2, q, s).start()
        return c

    lax.fori_loop(0, n_fs - 1, pass_down, 0)

    def mate_down(i, c):
        s = lax.rem(me + n_fs - turn(i), n_fs)
        y_copy(2, other, s).wait_recv()
        return c

    lax.fori_loop(0, n_fs - 1, mate_down, 0)
    outs[2].start()

    srcs = 4
    deep = srcs * per

    def outputs(i, c):
        rows = pl.ds(pl.multiple_of(i * deep, deep), deep)
        mix = jnp.zeros((deep, cols), F32)
        for k in range(2):
            acc = jnp.zeros((deep, cols), F32)
            for f in range(n_tp // 2):
                h = jnp.concatenate([h_buf[2 * f, k, rows], h_buf[2 * f + 1, k, rows]], axis=1)
                acc += jnp.dot(
                    h, od[k, 2 * f * width : 2 * (f + 1) * width], preferred_element_type=F32
                )
            w = w_rows[k, rows]
            mix += acc.astype(BF16).astype(F32) * jnp.concatenate([w] * (cols // 128), axis=1)
        mix = mix.astype(BF16)
        for b in range(srcs):
            for m in range(span):
                at = b * per + m * quarter
                spot = pl.ds(pl.multiple_of((i * srcs + b) * quarter, quarter), quarter)
                part[m, spot] = mix[at : at + quarter]
        return c

    lax.fori_loop(0, n_fs // srcs, outputs, 0)

    def part_copy(to_member, from_member):
        return remote(
            part.at[to_member], gathered.at[from_member], ps_sem.at[to_member], pr_sem.at[from_member],
            {"fs": base + to_member},
        )

    for i in range(1, span):
        part_copy(lax.rem(member + i, span), member).start()
    tot = part[member].astype(F32)
    for i in range(1, span):
        frm = lax.rem(member + span - i, span)
        part_copy(frm, frm).wait_recv()
        tot += gathered[frm].astype(F32)
    total[...] = tot.astype(BF16)

    def back_copy(j, s):
        return remote(
            total.at[pl.ds(pl.multiple_of(j * quarter, quarter), quarter)],
            final.at[pl.ds(pl.multiple_of(s * quarter, quarter), quarter)],
            fs_sem.at[j], fr_sem.at[s], {"fs": j},
        )

    def send_back(i, c):
        back_copy(lax.rem(me + turn(i), n_fs), me).start()
        return c

    lax.fori_loop(0, n_fs - 1, send_back, 0)
    here = pl.ds(pl.multiple_of(me * quarter, quarter), quarter)
    final[here] = total[here]

    def get_back(i, c):
        s = lax.rem(me + n_fs - turn(i), n_fs)
        back_copy(s, s).wait_recv()
        return c

    lax.fori_loop(0, n_fs - 1, get_back, 0)
    mix_ref[...] = jnp.dot(place, final[...], preferred_element_type=F32).astype(BF16)

    def drain(i, c):
        j = lax.rem(me + i, n_fs)
        tok_copy(j, me).wait_send()
        w_copy(j, me).wait_send()
        back_copy(j, me).wait_send()
        for a in range(3):
            z_copy(a, j, me).wait_send()
            y_copy(a, q, j).wait_send()
        return c

    lax.fori_loop(1, n_fs, drain, 0)
    for i in range(1, span):
        part_copy(lax.rem(member + i, span), member).wait_send()
    for copy in sent:
        copy.wait_send()
    for out in outs:
        out.wait()


def solution(mesh):
    n_fs, n_tp = mesh.shape["fs"], mesh.shape["tp"]

    def on_device(tokens, route_ids, route_weights, ffn_gain, gate_master, up_master, down_master):
        toks, d = tokens.shape
        experts, rows, width = gate_master.shape
        down_rows, cols = down_master.shape[1:]
        served = experts // n_fs
        span = GROUP_SIZE // served
        per = toks // (experts // GROUP_SIZE)
        all_rows = n_fs * per
        quarter = per // span
        dma = pltpu.SemaphoreType.DMA
        shape = jax.ShapeDtypeStruct
        vmem, hbm = pl.BlockSpec(memory_space=pltpu.VMEM), pl.BlockSpec(memory_space=pl.ANY)
        return tuple(
            pl.pallas_call(
                functools.partial(kernel, n_fs, n_tp, span),
                out_shape=(
                    shape((served, n_fs * rows, width), BF16),
                    shape((served, n_fs * rows, width), BF16),
                    shape((served, n_fs * down_rows, cols), BF16),
                    shape((toks, cols), BF16),
                ),
                in_specs=[vmem] * 4 + [hbm] * 3,
                out_specs=(hbm, hbm, hbm, vmem),
                scratch_shapes=[
                    pltpu.VMEM((n_fs, rows, width), F32),
                    pltpu.VMEM((n_fs, rows, width), F32),
                    pltpu.VMEM((n_fs, down_rows, cols), F32),
                    pltpu.VMEM((rows, width), F32),
                    pltpu.VMEM((rows, width), F32),
                    pltpu.VMEM((down_rows, cols), F32),
                    pltpu.VMEM((n_fs, rows, width), BF16),
                    pltpu.VMEM((n_fs, rows, width), BF16),
                    pltpu.VMEM((n_fs, down_rows, cols), BF16),
                    pltpu.VMEM((served, n_fs * rows, width), BF16),
                    pltpu.VMEM((served, n_fs * rows, width), BF16),
                    pltpu.VMEM((served, n_fs * down_rows, cols), BF16),
                    pltpu.VMEM((toks, cols), BF16),
                    pltpu.VMEM((n_fs, served, 128), F32),
                    pltpu.VMEM((n_tp, 2, all_rows // 2, cols), BF16),
                    pltpu.VMEM((n_fs, served, 128), F32),
                    pltpu.VMEM((n_tp, served, all_rows, width), BF16),
                    pltpu.VMEM((served, all_rows, 128), F32),
                    pltpu.VMEM((span, n_fs * quarter, cols), BF16),
                    pltpu.VMEM((span, n_fs * quarter, cols), BF16),
                    pltpu.VMEM((n_fs * quarter, cols), BF16),
                    pltpu.VMEM((n_fs * quarter, cols), BF16),
                    dma((6,)),
                    dma((3,)),
                    dma((3, n_fs)),
                    dma((3, n_fs)),
                    dma((3, n_fs)),
                    dma((3, n_fs)),
                    dma((2, n_fs)),
                    dma((2, n_fs)),
                    dma((8,)),
                    dma((8,)),
                    dma((8,)),
                    dma((8,)),
                    dma((span,)),
                    dma((span,)),
                    dma((n_fs,)),
                    dma((n_fs,)),
                ],
                compiler_params=pltpu.CompilerParams(
                    collective_id=0, has_side_effects=True, vmem_limit_bytes=56 * 1024 * 1024
                ),
                name="experts",
            )(
                tokens,
                route_ids,
                route_weights,
                ffn_gain.reshape(rows, 1),
                gate_master.reshape(n_fs, served, rows, width),
                up_master.reshape(n_fs, served, rows, width),
                down_master.reshape(n_fs, served, down_rows, cols),
            )
        )

    in_specs = (
        P(("grp", "fs"), None),
        P(("grp", "fs"), None),
        P(("grp", "fs"), None),
        P("fs"),
        P(None, "fs", "tp"),
        P(None, "fs", "tp"),
        P(None, "fs", "tp"),
    )
    out_specs = (
        P(("grp", "fs"), None, "tp"),
        P(("grp", "fs"), None, "tp"),
        P(("grp", "fs"), None, "tp"),
        P(("grp", "fs"), "tp"),
    )
    return jax.shard_map(
        on_device, mesh=mesh, in_specs=in_specs, out_specs=out_specs, check_vma=False
    )
```

```python
import functools

import jax
import jax.numpy as jnp
from jax import lax
from jax.experimental import pallas as pl
from jax.experimental.pallas import tpu as pltpu
from jax.sharding import PartitionSpec as P

GROUP_SIZE = 8
MESH = pl.DeviceIdType.MESH
BF16 = jnp.bfloat16
F32 = jnp.float32
PASS_GATE_UP = (6, 8)
PASS_DOWN = (5, 9)


def remote(src, dst, send, recv, where):
    return pltpu.make_async_remote_copy(
        src_ref=src, dst_ref=dst, send_sem=send, recv_sem=recv, device_id=where, device_id_type=MESH
    )


def kernel(
    n_fs, n_tp, span,
    tok_ref, ids_ref, rw_ref, gain_ref, gm_ref, um_ref, dm_ref,
    og, ou, od, mix_ref,
    g_in, u_in, d_in, g_own, u_own, d_own, g_send, u_send, d_send,
    s_buf, w_send, x_buf, w_recv, h_buf, w_rows, pick, spread, part, gathered, total, final,
    load_sem, z_send, z_recv, y_send, y_recv, w_sems, t_send, t_recv,
    xs_sem, xr_sem, hs_sem, hr_sem, ps_sem, pr_sem, fs_sem, fr_sem,
):
    grp, me, t = lax.axis_index("grp"), lax.axis_index("fs"), lax.axis_index("tp")
    q = lax.rem(grp, 2)
    other = 1 - q
    mate = grp + 1 - 2 * q
    right, left = lax.rem(t + 2, n_tp), lax.rem(t + n_tp - 2, n_tp)
    far = lax.rem(t + 4, n_tp)
    twin = t + 1 - 2 * lax.rem(t, 2)
    member = lax.rem(me, span)
    base = me - member
    groups = n_fs // span
    gid = lax.div(me, span)
    gnext, gprev, gopp = (lax.rem(gid + k, groups) for k in (1, groups - 1, groups // 2))
    toks = tok_ref.shape[0]
    cols = s_buf.shape[1]
    per = s_buf.shape[0] // groups
    quarter = per // span
    slots = per // 2

    def turn(i):
        half = lax.div(i, 2)
        odd = lax.rem(i, 2)
        return half + 1 + odd * (n_fs - 2 * half - 2)

    barrier = pltpu.get_barrier_semaphore()

    def greet(i, c):
        pl.semaphore_signal(
            barrier, inc=1, device_id={"fs": lax.rem(me + i, n_fs)}, device_id_type=MESH
        )
        return c

    lax.fori_loop(1, n_fs, greet, 0)
    pl.semaphore_signal(barrier, inc=1, device_id={"grp": mate}, device_id_type=MESH)
    for peer in (right, left, twin):
        pl.semaphore_signal(barrier, inc=1, device_id={"tp": peer}, device_id_type=MESH)

    loads = [
        pltpu.make_async_copy(gm_ref.at[:, q], g_in, load_sem.at[0]),
        pltpu.make_async_copy(um_ref.at[:, q], u_in, load_sem.at[1]),
        pltpu.make_async_copy(dm_ref.at[:, q], d_in, load_sem.at[2]),
        pltpu.make_async_copy(gm_ref.at[me, other], g_own, load_sem.at[3]),
        pltpu.make_async_copy(um_ref.at[me, other], u_own, load_sem.at[4]),
        pltpu.make_async_copy(dm_ref.at[me, other], d_own, load_sem.at[5]),
    ]
    for load in loads:
        load.start()

    ids = ids_ref[...]
    first, second = ids[0:1], ids[1:2]
    group = lax.shift_right_logical(first, GROUP_SIZE.bit_length() - 1)
    group_hot = (group == lax.broadcasted_iota(jnp.int32, (8, toks), 0)).astype(F32)
    row = lax.broadcasted_iota(jnp.int32, (toks, toks), 0)
    col = lax.broadcasted_iota(jnp.int32, (toks, toks), 1)
    counts = jnp.dot(
        group_hot.astype(BF16), (row < col).astype(BF16), preferred_element_type=F32
    )
    rank = jnp.sum(counts * group_hot, axis=0, keepdims=True)
    target = group.astype(F32) * per + rank
    place = (target == row.astype(F32)).astype(BF16)
    tok = tok_ref[...].astype(F32)
    scale = lax.rsqrt(jnp.mean(tok * tok, axis=1, keepdims=True) + 1e-06)
    own = tok_ref[:, pl.ds(pl.multiple_of(t * cols, cols), cols)].astype(F32)
    normed = (own * scale).astype(BF16)
    s_buf[...] = jnp.dot(place, normed, preferred_element_type=F32).astype(BF16)
    rw = rw_ref[...]
    expert = lax.broadcasted_iota(jnp.int32, (2 * n_fs, toks), 0)
    by_expert = jnp.where(first == expert, rw[0:1], 0.0) + jnp.where(second == expert, rw[1:2], 0.0)
    rank_hot = (rank == lax.broadcasted_iota(jnp.int32, (128, toks), 0).astype(F32)).astype(F32)
    w_all = lax.dot_general(
        by_expert, rank_hot, (((1,), (1,)), ((), ())),
        preferred_element_type=F32, precision=lax.Precision.HIGHEST,
    )
    for j in range(n_fs):
        w_send[j] = w_all[2 * j : 2 * j + 2]

    pl.semaphore_wait(barrier, n_fs - 1 + 4)

    x_half = x_buf.shape[2] // per

    def rows_at(s):
        return x_buf.at[
            t, lax.div(s, x_half), pl.ds(pl.multiple_of(lax.rem(s, x_half) * per, per), per)
        ]

    def row_copy(j, s):
        begin = pl.multiple_of(lax.div(j, span) * per, per)
        return remote(
            s_buf.at[pl.ds(begin, per)], rows_at(s), t_send.at[j], t_recv.at[s], {"fs": j}
        )

    def w_copy(j, s):
        return remote(w_send.at[j], w_recv.at[s], w_sems.at[0, j], w_sems.at[1, s], {"fs": j})

    def dispatch(i, c):
        j = lax.rem(me + turn(i), n_fs)
        row_copy(j, me).start()
        w_copy(j, me).start()
        return c

    lax.fori_loop(0, n_fs - 1, dispatch, 0)

    gain_row = gain_ref[...]
    side = gain_row.shape[1]
    diagonal = lax.broadcasted_iota(jnp.int32, (side, side), 0) == lax.broadcasted_iota(
        jnp.int32, (side, side), 1
    )
    gain = jnp.broadcast_to(
        jnp.sum(jnp.where(diagonal, gain_row, 0.0), axis=1, keepdims=True), g_own.shape
    )
    gate_rows, down_rows = g_own.shape[0], d_own.shape[0]

    def gate_at(buf, e, s):
        return buf.at[e, pl.ds(pl.multiple_of(s * gate_rows, gate_rows), gate_rows)]

    def down_at(buf, e, s):
        return buf.at[e, pl.ds(pl.multiple_of(s * down_rows, down_rows), down_rows)]

    def z_copy(a, j, s):
        src = (g_send, u_send, d_send)[a].at[j]
        dst = (gate_at(og, q, s), gate_at(ou, q, s), down_at(od, q, s))[a]
        return remote(src, dst, z_send.at[a, j], z_recv.at[a, s], {"fs": j})

    def y_copy(a, e, s):
        spot = (gate_at(og, e, s), gate_at(ou, e, s), down_at(od, e, s))[a]
        return remote(spot, spot, y_send.at[a, s], y_recv.at[a, s], {"grp": mate})

    def send_gate_up(i, c):
        j = lax.rem(me + turn(i), n_fs)
        g_send[j] = (g_in[j] * gain).astype(BF16)
        u_send[j] = (u_in[j] * gain).astype(BF16)
        z_copy(0, j, me).start()
        z_copy(1, j, me).start()
        return c

    def send_down(i, c):
        j = lax.rem(me + turn(i), n_fs)
        d_send[j] = d_in[j].astype(BF16)
        z_copy(2, j, me).start()
        return c

    def pass_on(arrays, begin, end):
        def one(i, c):
            s = lax.rem(me + n_fs - turn(i), n_fs)
            for a in arrays:
                z_copy(a, s, s).wait_recv()
                y_copy(a, q, s).start()
            return c

        lax.fori_loop(begin, end, one, 0)

    def from_mate(arrays):
        def one(i, c):
            s = lax.rem(me + n_fs - turn(i), n_fs)
            for a in arrays:
                y_copy(a, other, s).wait_recv()
            return c

        lax.fori_loop(0, n_fs - 1, one, 0)

    last = n_fs - 1
    loads[0].wait()
    loads[1].wait()
    lax.fori_loop(0, last, send_gate_up, 0)
    for load in loads[2:]:
        load.wait()
    lax.fori_loop(0, last, send_down, 0)
    own_rows = s_buf[pl.ds(pl.multiple_of(gid * per, per), per)]
    x_buf[t, lax.div(me, x_half), pl.ds(pl.multiple_of(lax.rem(me, x_half) * per, per), per)] = own_rows
    w_recv[me] = w_send[me]

    def tp_gather(buf, send, recv, between):
        def to(block, k, peer):
            return remote(block, block, send.at[k], recv.at[k], {"tp": peer})

        one = [to(buf.at[t], 0, right), to(buf.at[t], 1, left), to(buf.at[t], 4, twin)]
        for copy in one:
            copy.start()
        between[0]()
        to(buf.at[left], 0, right).wait_recv()
        two = [to(buf.at[left, 0], 2, right), to(buf.at[left], 5, twin)]
        for copy in two:
            copy.start()
        to(buf.at[right], 1, left).wait_recv()
        three = [to(buf.at[right, 1], 3, left), to(buf.at[right], 6, twin)]
        for copy in three:
            copy.start()
        between[1]()
        to(buf.at[far, 0], 2, right).wait_recv()
        to(buf.at[far, 1], 3, left).wait_recv()
        four = [to(buf.at[far], 7, twin)]
        four[0].start()
        between[2]()
        for k, shift in ((4, 0), (5, n_tp - 2), (6, 2), (7, 4)):
            to(buf.at[lax.rem(twin + shift, n_tp)], k, twin).wait_recv()
        return one + two + three + four

    eye = (
        lax.broadcasted_iota(jnp.int32, (per, 128), 0) == lax.broadcasted_iota(jnp.int32, (per, 128), 1)
    ).astype(F32)
    before = (
        lax.broadcasted_iota(jnp.int32, (128, 128), 0) < lax.broadcasted_iota(jnp.int32, (128, 128), 1)
    ).astype(BF16)
    slot_down = lax.broadcasted_iota(jnp.int32, (slots, 128), 0).astype(F32)
    slot_along = lax.broadcasted_iota(jnp.int32, (per, 128), 1).astype(F32)

    def index_rows():
        def one(s, c):
            both = w_recv[s]
            used = both > 0.0
            at = jnp.dot(used.astype(BF16), before, preferred_element_type=F32)
            at = jnp.where(used, at, -1.0)
            for k in range(2):
                pick[2 * s + k] = (at[k : k + 1] == slot_down).astype(BF16)
                column = jnp.sum(eye * both[k : k + 1], axis=1, keepdims=True)
                w_rows[k, pl.ds(pl.multiple_of(s * per, per), per)] = jnp.broadcast_to(column, (per, 128))
                at_col = jnp.sum(eye * at[k : k + 1], axis=1, keepdims=True)
                spread[2 * s + k] = (at_col == slot_along).astype(BF16)
            return c

        lax.fori_loop(0, n_fs, one, 0)

    def own_blocks():
        gate_spot = pl.ds(pl.multiple_of(me * gate_rows, gate_rows), gate_rows)
        down_spot = pl.ds(pl.multiple_of(me * down_rows, down_rows), down_rows)
        og[q, gate_spot] = (g_in[me] * gain).astype(BF16)
        ou[q, gate_spot] = (u_in[me] * gain).astype(BF16)
        od[q, down_spot] = d_in[me].astype(BF16)
        og[other, gate_spot] = (g_own[...] * gain).astype(BF16)
        ou[other, gate_spot] = (u_own[...] * gain).astype(BF16)
        od[other, down_spot] = d_own[...].astype(BF16)

    def rows_in(i, c):
        s = lax.rem(me + n_fs - turn(i), n_fs)
        row_copy(s, s).wait_recv()
        w_copy(s, s).wait_recv()
        return c

    own_blocks()
    lax.fori_loop(0, last, rows_in, 0)

    def while_x():
        index_rows()
        pass_on((0, 1), 0, PASS_GATE_UP[0])

    sent = tp_gather(
        x_buf, xs_sem, xr_sem,
        (
            while_x,
            lambda: pass_on((0, 1), PASS_GATE_UP[0], PASS_GATE_UP[1]),
            lambda: pass_on((0, 1), PASS_GATE_UP[1], last),
        ),
    )
    from_mate((0, 1))

    width = og.shape[2]
    tile = x_buf.shape[2]

    def hidden(i, c):
        half, k = lax.div(i, 2), lax.rem(i, 2)
        acc = jnp.zeros((tile, 2 * width), F32)
        for f in range(n_tp):
            w = jnp.concatenate(
                [og[k, f * cols : (f + 1) * cols], ou[k, f * cols : (f + 1) * cols]], axis=1
            )
            acc += jnp.dot(x_buf[f, half], w, preferred_element_type=F32)
        g, u = acc[:, :width], acc[:, width:]
        act = (g / (1.0 + jnp.exp(-g)) * u).astype(BF16)
        for b in range(tile // per):
            s = half * x_half + b
            rows = jnp.dot(
                pick[2 * s + k][:, :per], act[b * per : (b + 1) * per], preferred_element_type=F32
            )
            h_buf[t, k, pl.ds(pl.multiple_of(s * slots, slots), slots)] = rows.astype(BF16)
        return c

    lax.fori_loop(0, 4, hidden, 0)
    sent += tp_gather(
        h_buf, hs_sem, hr_sem,
        (
            lambda: pass_on((2,), 0, PASS_DOWN[0]),
            lambda: pass_on((2,), PASS_DOWN[0], PASS_DOWN[1]),
            lambda: pass_on((2,), PASS_DOWN[1], last),
        ),
    )
    from_mate((2,))

    deep = span * slots

    def outputs(sg):
        rows = pl.ds(pl.multiple_of(sg * deep, deep), deep)
        outs = []
        for k in range(2):
            acc = jnp.zeros((deep, cols), F32)
            for f in range(n_tp // 2):
                h = jnp.concatenate([h_buf[2 * f, k, rows], h_buf[2 * f + 1, k, rows]], axis=1)
                acc += jnp.dot(
                    h, od[k, 2 * f * width : 2 * (f + 1) * width], preferred_element_type=F32
                )
            outs.append(acc.astype(BF16))
        for b in range(span):
            s = sg * span + b
            mix = jnp.zeros((per, cols), F32)
            for k in range(2):
                full = jnp.dot(
                    spread[2 * s + k][:, :slots], outs[k][b * slots : (b + 1) * slots],
                    preferred_element_type=F32,
                )
                w = w_rows[k, pl.ds(pl.multiple_of(s * per, per), per)]
                mix += full * jnp.concatenate([w] * (cols // 128), axis=1)
            mix = mix.astype(BF16)
            for m in range(span):
                part[sg, m, b * quarter : (b + 1) * quarter] = mix[m * quarter : (m + 1) * quarter]

    def part_copy(sg, to_member, from_member):
        return remote(
            part.at[sg, to_member], gathered.at[sg, from_member],
            ps_sem.at[sg, to_member], pr_sem.at[sg, from_member], {"fs": base + to_member},
        )

    def back_copy(sg, b, s):
        return remote(
            total.at[sg, b * quarter : (b + 1) * quarter],
            final.at[pl.ds(pl.multiple_of(s * quarter, quarter), quarter)],
            fs_sem.at[sg, b], fr_sem.at[s], {"fs": sg * span + b},
        )

    order = (gopp, gnext, gprev, gid)
    for sg in order:
        outputs(sg)
        for i in range(1, span):
            part_copy(sg, lax.rem(member + i, span), member).start()
    for sg in order:
        tot = part[sg, member].astype(F32)
        for i in range(1, span):
            frm = lax.rem(member + span - i, span)
            part_copy(sg, frm, frm).wait_recv()
            tot += gathered[sg, frm].astype(F32)
        total[sg] = tot.astype(BF16)
        for b in range(span):
            if sg is not gid:
                back_copy(sg, b, me).start()
            else:

                @pl.when(member != b)
                def _():
                    back_copy(sg, b, me).start()

    here = pl.ds(pl.multiple_of(me * quarter, quarter), quarter)
    final[here] = total[gid, pl.ds(pl.multiple_of(member * quarter, quarter), quarter)]

    def get_back(i, c):
        s = lax.rem(me + n_fs - turn(i), n_fs)
        remote(final.at[here], final.at[here], fr_sem.at[s], fr_sem.at[s], {"fs": s}).wait_recv()
        return c

    lax.fori_loop(0, last, get_back, 0)
    mix_ref[...] = lax.dot_general(
        place, final[...], (((0,), (0,)), ((), ())), preferred_element_type=F32
    ).astype(BF16)

    def drain(i, c):
        j = lax.rem(me + i, n_fs)
        row_copy(j, me).wait_send()
        w_copy(j, me).wait_send()
        for a in range(3):
            z_copy(a, j, me).wait_send()
            y_copy(a, q, j).wait_send()
        return c

    lax.fori_loop(1, n_fs, drain, 0)
    for sg in order:
        for i in range(1, span):
            part_copy(sg, lax.rem(member + i, span), member).wait_send()
        for b in range(span):
            if sg is not gid:
                back_copy(sg, b, me).wait_send()
            else:

                @pl.when(member != b)
                def _():
                    back_copy(sg, b, me).wait_send()

    for copy in sent:
        copy.wait_send()


def write_out(*refs):
    half = len(refs) // 2
    ins, outs, sems = refs[:half], refs[half : 2 * half], refs[2 * half]
    copies = [pltpu.make_async_copy(a, b, sems.at[i]) for i, (a, b) in enumerate(zip(ins, outs))]
    for copy in copies:
        copy.start()
    for copy in copies:
        copy.wait()


def solution(mesh):
    n_fs, n_tp = mesh.shape["fs"], mesh.shape["tp"]

    def on_device(tokens, route_ids, route_weights, ffn_gain, gate_master, up_master, down_master):
        toks, d = tokens.shape
        experts, rows, width = gate_master.shape
        down_rows, cols = down_master.shape[1:]
        served = experts // n_fs
        span = GROUP_SIZE // served
        per = toks // (experts // GROUP_SIZE)
        all_rows = n_fs * per
        quarter = per // span
        dma = pltpu.SemaphoreType.DMA
        shape = jax.ShapeDtypeStruct
        vmem, hbm = pl.BlockSpec(memory_space=pltpu.VMEM), pl.BlockSpec(memory_space=pl.ANY)
        groups = n_fs // span
        out_shape = (
            shape((served, n_fs * rows, width), BF16),
            shape((served, n_fs * rows, width), BF16),
            shape((served, n_fs * down_rows, cols), BF16),
            shape((toks, cols), BF16),
        )
        results = pl.pallas_call(
            functools.partial(kernel, n_fs, n_tp, span),
            out_shape=out_shape,
            in_specs=[vmem] * 4 + [hbm] * 3,
            out_specs=(vmem,) * 4,
            scratch_shapes=[
                pltpu.VMEM((n_fs, rows, width), F32),
                pltpu.VMEM((n_fs, rows, width), F32),
                pltpu.VMEM((n_fs, down_rows, cols), F32),
                pltpu.VMEM((rows, width), F32),
                pltpu.VMEM((rows, width), F32),
                pltpu.VMEM((down_rows, cols), F32),
                pltpu.VMEM((n_fs, rows, width), BF16),
                pltpu.VMEM((n_fs, rows, width), BF16),
                pltpu.VMEM((n_fs, down_rows, cols), BF16),
                pltpu.VMEM((toks, cols), BF16),
                pltpu.VMEM((n_fs, served, 128), F32),
                pltpu.VMEM((n_tp, 2, all_rows // 2, cols), BF16),
                pltpu.VMEM((n_fs, served, 128), F32),
                pltpu.VMEM((n_tp, served, all_rows // 2, width), BF16),
                pltpu.VMEM((served, all_rows, 128), F32),
                pltpu.VMEM((n_fs * served, per // 2, 128), BF16),
                pltpu.VMEM((n_fs * served, per, 128), BF16),
                pltpu.VMEM((groups, span, span * quarter, cols), BF16),
                pltpu.VMEM((groups, span, span * quarter, cols), BF16),
                pltpu.VMEM((groups, span * quarter, cols), BF16),
                pltpu.VMEM((n_fs * quarter, cols), BF16),
                dma((6,)),
                dma((3, n_fs)),
                dma((3, n_fs)),
                dma((3, n_fs)),
                dma((3, n_fs)),
                dma((2, n_fs)),
                dma((n_fs,)),
                dma((n_fs,)),
                dma((8,)),
                dma((8,)),
                dma((8,)),
                dma((8,)),
                dma((groups, span)),
                dma((groups, span)),
                dma((groups, span)),
                dma((n_fs,)),
            ],
            compiler_params=pltpu.CompilerParams(
                collective_id=0, has_side_effects=True, vmem_limit_bytes=50 * 1024 * 1024
            ),
            name="experts",
        )(
            tokens,
            route_ids.T,
            route_weights.T,
            ffn_gain.reshape(1, rows),
            gate_master.reshape(n_fs, served, rows, width),
            up_master.reshape(n_fs, served, rows, width),
            down_master.reshape(n_fs, served, down_rows, cols),
        )
        return tuple(
            pl.pallas_call(
                write_out,
                out_shape=out_shape,
                in_specs=[vmem] * 4,
                out_specs=(hbm,) * 4,
                scratch_shapes=[dma((4,))],
                compiler_params=pltpu.CompilerParams(vmem_limit_bytes=8 * 1024 * 1024),
                name="write_out",
            )(*results)
        )

    in_specs = (
        P(("grp", "fs"), None),
        P(("grp", "fs"), None),
        P(("grp", "fs"), None),
        P("fs"),
        P(None, "fs", "tp"),
        P(None, "fs", "tp"),
        P(None, "fs", "tp"),
    )
    out_specs = (
        P(("grp", "fs"), None, "tp"),
        P(("grp", "fs"), None, "tp"),
        P(("grp", "fs"), None, "tp"),
        P(("grp", "fs"), "tp"),
    )
    return jax.shard_map(
        on_device, mesh=mesh, in_specs=in_specs, out_specs=out_specs, check_vma=False
    )
```

```python
import functools

import jax
import jax.numpy as jnp
from jax import lax
from jax.experimental import pallas as pl
from jax.experimental.pallas import tpu as pltpu
from jax.sharding import PartitionSpec as P

GROUP_SIZE = 8
MESH = pl.DeviceIdType.MESH
BF16 = jnp.bfloat16
F32 = jnp.float32
PASS_GATE_UP = (6, 8)
PASS_DOWN = (5, 9)


def remote(src, dst, send, recv, where):
    return pltpu.make_async_remote_copy(
        src_ref=src, dst_ref=dst, send_sem=send, recv_sem=recv, device_id=where, device_id_type=MESH
    )


def kernel(
    n_fs, n_tp, span,
    tok_hbm, ids_hbm, rw_hbm, gain_hbm, gm_ref, um_ref, dm_ref,
    og, ou, od, mix_ref,
    tok_ref, ids_ref, rw_ref, gain_ref, own_part, own_in,
    g_in, u_in, d_in, g_own, u_own, d_own, g_send, u_send, d_send,
    s_buf, w_send, x_buf, w_recv, h_buf, w_rows, pick, spread, part, gathered, total, final,
    load_sem, z_send, z_recv, y_send, y_recv, w_sems, t_send, t_recv,
    xs_sem, xr_sem, hs_sem, hr_sem, ps_sem, pr_sem, fs_sem, fr_sem,
):
    grp, me, t = lax.axis_index("grp"), lax.axis_index("fs"), lax.axis_index("tp")
    q = lax.rem(grp, 2)
    other = 1 - q
    mate = grp + 1 - 2 * q
    right, left = lax.rem(t + 2, n_tp), lax.rem(t + n_tp - 2, n_tp)
    far = lax.rem(t + 4, n_tp)
    twin = t + 1 - 2 * lax.rem(t, 2)
    member = lax.rem(me, span)
    base = me - member
    groups = n_fs // span
    gid = lax.div(me, span)
    gnext, gprev, gopp = (lax.rem(gid + k, groups) for k in (1, groups - 1, groups // 2))
    toks = tok_ref.shape[0]
    cols = s_buf.shape[1]
    per = s_buf.shape[0] // groups
    quarter = per // span
    slots = per // 2

    def turn(i):
        half = lax.div(i, 2)
        odd = lax.rem(i, 2)
        return half + 1 + odd * (n_fs - 2 * half - 2)

    barrier = pltpu.get_barrier_semaphore()

    def greet(i, c):
        pl.semaphore_signal(
            barrier, inc=1, device_id={"fs": lax.rem(me + i, n_fs)}, device_id_type=MESH
        )
        return c

    lax.fori_loop(1, n_fs, greet, 0)
    pl.semaphore_signal(barrier, inc=1, device_id={"grp": mate}, device_id_type=MESH)
    for peer in (right, left, twin):
        pl.semaphore_signal(barrier, inc=1, device_id={"tp": peer}, device_id_type=MESH)

    loads = [
        pltpu.make_async_copy(gm_ref.at[:, q], g_in, load_sem.at[0]),
        pltpu.make_async_copy(um_ref.at[:, q], u_in, load_sem.at[1]),
        pltpu.make_async_copy(dm_ref.at[:, q], d_in, load_sem.at[2]),
        pltpu.make_async_copy(gm_ref.at[me, other], g_own, load_sem.at[3]),
        pltpu.make_async_copy(um_ref.at[me, other], u_own, load_sem.at[4]),
        pltpu.make_async_copy(dm_ref.at[me, other], d_own, load_sem.at[5]),
    ]
    small = [
        pltpu.make_async_copy(a, b, load_sem.at[6 + i])
        for i, (a, b) in enumerate(
            ((ids_hbm, ids_ref), (rw_hbm, rw_ref), (gain_hbm, gain_ref), (tok_hbm, tok_ref))
        )
    ]
    for load in small + loads:
        load.start()

    for load in small:
        load.wait()
    ids = ids_ref[...]
    first, second = ids[0:1], ids[1:2]
    group = lax.shift_right_logical(first, GROUP_SIZE.bit_length() - 1)
    group_hot = (group == lax.broadcasted_iota(jnp.int32, (8, toks), 0)).astype(F32)
    row = lax.broadcasted_iota(jnp.int32, (toks, toks), 0)
    col = lax.broadcasted_iota(jnp.int32, (toks, toks), 1)
    counts = jnp.dot(
        group_hot.astype(BF16), (row < col).astype(BF16), preferred_element_type=F32
    )
    rank = jnp.sum(counts * group_hot, axis=0, keepdims=True)
    target = group.astype(F32) * per + rank
    place = (target == row.astype(F32)).astype(BF16)
    tok = tok_ref[...].astype(F32)
    scale = lax.rsqrt(jnp.mean(tok * tok, axis=1, keepdims=True) + 1e-06)
    own = tok_ref[:, pl.ds(pl.multiple_of(t * cols, cols), cols)].astype(F32)
    normed = (own * scale).astype(BF16)
    s_buf[...] = jnp.dot(place, normed, preferred_element_type=F32).astype(BF16)
    rw = rw_ref[...]
    expert = lax.broadcasted_iota(jnp.int32, (2 * n_fs, toks), 0)
    by_expert = jnp.where(first == expert, rw[0:1], 0.0) + jnp.where(second == expert, rw[1:2], 0.0)
    rank_hot = (rank == lax.broadcasted_iota(jnp.int32, (128, toks), 0).astype(F32)).astype(F32)
    w_all = lax.dot_general(
        by_expert, rank_hot, (((1,), (1,)), ((), ())),
        preferred_element_type=F32, precision=lax.Precision.HIGHEST,
    )
    for j in range(n_fs):
        w_send[j] = w_all[2 * j : 2 * j + 2]

    pl.semaphore_wait(barrier, n_fs - 1 + 4)

    x_half = x_buf.shape[2] // per

    def rows_at(s):
        return x_buf.at[
            t, lax.div(s, x_half), pl.ds(pl.multiple_of(lax.rem(s, x_half) * per, per), per)
        ]

    def row_copy(j, s):
        begin = pl.multiple_of(lax.div(j, span) * per, per)
        return remote(
            s_buf.at[pl.ds(begin, per)], rows_at(s), t_send.at[j], t_recv.at[s], {"fs": j}
        )

    def w_copy(j, s):
        return remote(w_send.at[j], w_recv.at[s], w_sems.at[0, j], w_sems.at[1, s], {"fs": j})

    def dispatch(i, c):
        j = lax.rem(me + turn(i), n_fs)
        row_copy(j, me).start()
        w_copy(j, me).start()
        return c

    lax.fori_loop(0, n_fs - 1, dispatch, 0)

    gain_row = gain_ref[...]
    side = gain_row.shape[1]
    diagonal = lax.broadcasted_iota(jnp.int32, (side, side), 0) == lax.broadcasted_iota(
        jnp.int32, (side, side), 1
    )
    gain = jnp.broadcast_to(
        jnp.sum(jnp.where(diagonal, gain_row, 0.0), axis=1, keepdims=True), g_own.shape
    )
    gate_rows, down_rows = g_own.shape[0], d_own.shape[0]

    def gate_at(buf, e, s):
        return buf.at[e, pl.ds(pl.multiple_of(s * gate_rows, gate_rows), gate_rows)]

    def down_at(buf, e, s):
        return buf.at[e, pl.ds(pl.multiple_of(s * down_rows, down_rows), down_rows)]

    def z_copy(a, j, s):
        src = (g_send, u_send, d_send)[a].at[j]
        dst = (gate_at(og, q, s), gate_at(ou, q, s), down_at(od, q, s))[a]
        return remote(src, dst, z_send.at[a, j], z_recv.at[a, s], {"fs": j})

    def y_copy(a, e, s):
        spot = (gate_at(og, e, s), gate_at(ou, e, s), down_at(od, e, s))[a]
        return remote(spot, spot, y_send.at[a, s], y_recv.at[a, s], {"grp": mate})

    def send_gate_up(i, c):
        j = lax.rem(me + turn(i), n_fs)
        g_send[j] = (g_in[j] * gain).astype(BF16)
        u_send[j] = (u_in[j] * gain).astype(BF16)
        z_copy(0, j, me).start()
        z_copy(1, j, me).start()
        return c

    def send_down(i, c):
        j = lax.rem(me + turn(i), n_fs)
        d_send[j] = d_in[j].astype(BF16)
        z_copy(2, j, me).start()
        return c

    def pass_on(arrays, begin, end):
        def one(i, c):
            s = lax.rem(me + n_fs - turn(i), n_fs)
            for a in arrays:
                z_copy(a, s, s).wait_recv()
                y_copy(a, q, s).start()
            return c

        lax.fori_loop(begin, end, one, 0)

    def from_mate(arrays):
        def one(i, c):
            s = lax.rem(me + n_fs - turn(i), n_fs)
            for a in arrays:
                y_copy(a, other, s).wait_recv()
            return c

        lax.fori_loop(0, n_fs - 1, one, 0)

    last = n_fs - 1
    loads[0].wait()
    loads[1].wait()
    lax.fori_loop(0, last, send_gate_up, 0)
    for load in loads[2:]:
        load.wait()
    lax.fori_loop(0, last, send_down, 0)
    own_rows = s_buf[pl.ds(pl.multiple_of(gid * per, per), per)]
    x_buf[t, lax.div(me, x_half), pl.ds(pl.multiple_of(lax.rem(me, x_half) * per, per), per)] = own_rows
    w_recv[me] = w_send[me]

    def tp_gather(buf, send, recv, between):
        def to(block, k, peer):
            return remote(block, block, send.at[k], recv.at[k], {"tp": peer})

        one = [to(buf.at[t], 0, right), to(buf.at[t], 1, left), to(buf.at[t], 4, twin)]
        for copy in one:
            copy.start()
        between[0]()
        to(buf.at[left], 0, right).wait_recv()
        two = [to(buf.at[left, 0], 2, right), to(buf.at[left], 5, twin)]
        for copy in two:
            copy.start()
        to(buf.at[right], 1, left).wait_recv()
        three = [to(buf.at[right, 1], 3, left), to(buf.at[right], 6, twin)]
        for copy in three:
            copy.start()
        between[1]()
        to(buf.at[far, 0], 2, right).wait_recv()
        to(buf.at[far, 1], 3, left).wait_recv()
        four = [to(buf.at[far], 7, twin)]
        four[0].start()
        between[2]()
        for k, shift in ((4, 0), (5, n_tp - 2), (6, 2), (7, 4)):
            to(buf.at[lax.rem(twin + shift, n_tp)], k, twin).wait_recv()
        return one + two + three + four

    eye = (
        lax.broadcasted_iota(jnp.int32, (per, 128), 0) == lax.broadcasted_iota(jnp.int32, (per, 128), 1)
    ).astype(F32)
    before = (
        lax.broadcasted_iota(jnp.int32, (128, 128), 0) < lax.broadcasted_iota(jnp.int32, (128, 128), 1)
    ).astype(BF16)
    slot_down = lax.broadcasted_iota(jnp.int32, (slots, 128), 0).astype(F32)
    slot_along = lax.broadcasted_iota(jnp.int32, (per, 128), 1).astype(F32)

    def index_rows():
        def one(s, c):
            both = w_recv[s]
            used = both > 0.0
            at = jnp.dot(used.astype(BF16), before, preferred_element_type=F32)
            at = jnp.where(used, at, -1.0)
            for k in range(2):
                pick[2 * s + k] = (at[k : k + 1] == slot_down).astype(BF16)
                column = jnp.sum(eye * both[k : k + 1], axis=1, keepdims=True)
                w_rows[k, pl.ds(pl.multiple_of(s * per, per), per)] = jnp.broadcast_to(column, (per, 128))
                at_col = jnp.sum(eye * at[k : k + 1], axis=1, keepdims=True)
                spread[2 * s + k] = (at_col == slot_along).astype(BF16)
            return c

        lax.fori_loop(0, n_fs, one, 0)

    def own_blocks():
        gate_spot = pl.ds(pl.multiple_of(me * gate_rows, gate_rows), gate_rows)
        down_spot = pl.ds(pl.multiple_of(me * down_rows, down_rows), down_rows)
        og[q, gate_spot] = (g_in[me] * gain).astype(BF16)
        ou[q, gate_spot] = (u_in[me] * gain).astype(BF16)
        od[q, down_spot] = d_in[me].astype(BF16)
        og[other, gate_spot] = (g_own[...] * gain).astype(BF16)
        ou[other, gate_spot] = (u_own[...] * gain).astype(BF16)
        od[other, down_spot] = d_own[...].astype(BF16)

    def rows_in(i, c):
        s = lax.rem(me + n_fs - turn(i), n_fs)
        row_copy(s, s).wait_recv()
        w_copy(s, s).wait_recv()
        return c

    own_blocks()
    lax.fori_loop(0, last, rows_in, 0)

    def while_x():
        index_rows()
        pass_on((0, 1), 0, PASS_GATE_UP[0])

    sent = tp_gather(
        x_buf, xs_sem, xr_sem,
        (
            while_x,
            lambda: pass_on((0, 1), PASS_GATE_UP[0], PASS_GATE_UP[1]),
            lambda: pass_on((0, 1), PASS_GATE_UP[1], last),
        ),
    )
    from_mate((0, 1))

    width = og.shape[2]
    tile = x_buf.shape[2]

    def hidden(i, c):
        half, k = lax.div(i, 2), lax.rem(i, 2)
        acc = jnp.zeros((tile, 2 * width), F32)
        for f in range(n_tp):
            w = jnp.concatenate(
                [og[k, f * cols : (f + 1) * cols], ou[k, f * cols : (f + 1) * cols]], axis=1
            )
            acc += jnp.dot(x_buf[f, half], w, preferred_element_type=F32)
        g, u = acc[:, :width], acc[:, width:]
        act = (g / (1.0 + jnp.exp(-g)) * u).astype(BF16)
        for b in range(tile // per):
            s = half * x_half + b
            rows = jnp.dot(
                pick[2 * s + k][:, :per], act[b * per : (b + 1) * per], preferred_element_type=F32
            )
            h_buf[t, k, pl.ds(pl.multiple_of(s * slots, slots), slots)] = rows.astype(BF16)
        return c

    lax.fori_loop(0, 4, hidden, 0)
    sent += tp_gather(
        h_buf, hs_sem, hr_sem,
        (
            lambda: pass_on((2,), 0, PASS_DOWN[0]),
            lambda: pass_on((2,), PASS_DOWN[0], PASS_DOWN[1]),
            lambda: pass_on((2,), PASS_DOWN[1], last),
        ),
    )
    from_mate((2,))

    deep = span * slots

    def outputs(sg):
        rows = pl.ds(pl.multiple_of(sg * deep, deep), deep)
        outs = []
        for k in range(2):
            acc = jnp.zeros((deep, cols), F32)
            for f in range(n_tp // 2):
                h = jnp.concatenate([h_buf[2 * f, k, rows], h_buf[2 * f + 1, k, rows]], axis=1)
                acc += jnp.dot(
                    h, od[k, 2 * f * width : 2 * (f + 1) * width], preferred_element_type=F32
                )
            outs.append(acc.astype(BF16))
        for b in range(span):
            s = sg * span + b
            mix = jnp.zeros((per, cols), F32)
            for k in range(2):
                full = jnp.dot(
                    spread[2 * s + k][:, :slots], outs[k][b * slots : (b + 1) * slots],
                    preferred_element_type=F32,
                )
                w = w_rows[k, pl.ds(pl.multiple_of(s * per, per), per)]
                mix += full * jnp.concatenate([w] * (cols // 128), axis=1)
            mix = mix.astype(BF16)
            if sg is gid:
                own_part[b] = mix
                continue
            for m in range(span):
                part[sg, m, b * quarter : (b + 1) * quarter] = mix[m * quarter : (m + 1) * quarter]

    def part_copy(sg, to_member, from_member):
        direct = sg is gid
        return remote(
            own_part.at[to_member] if direct else part.at[sg, to_member],
            own_in.at[from_member] if direct else gathered.at[sg, from_member],
            ps_sem.at[sg, to_member], pr_sem.at[sg, from_member], {"fs": base + to_member},
        )

    def back_copy(sg, b, s):
        return remote(
            total.at[sg, b * quarter : (b + 1) * quarter],
            final.at[pl.ds(pl.multiple_of(s * quarter, quarter), quarter)],
            fs_sem.at[sg, b], fr_sem.at[s], {"fs": sg * span + b},
        )

    abroad = (gopp, gnext, gprev)
    for sg in abroad:
        outputs(sg)
        for i in range(1, span):
            part_copy(sg, lax.rem(member + i, span), member).start()
    outputs(gid)
    for sg in abroad:
        tot = part[sg, member].astype(F32)
        for i in range(1, span):
            frm = lax.rem(member + span - i, span)
            part_copy(sg, frm, frm).wait_recv()
            tot += gathered[sg, frm].astype(F32)
        total[sg] = tot.astype(BF16)
        for b in range(span):
            back_copy(sg, b, me).start()
        if sg is gopp:
            for i in range(1, span):
                part_copy(gid, lax.rem(member + i, span), member).start()

    tot = own_part[member].astype(F32)
    for i in range(1, span):
        frm = lax.rem(member + span - i, span)
        part_copy(gid, frm, frm).wait_recv()
        tot += own_in[frm].astype(F32)
    final[pl.ds(pl.multiple_of(gid * per, per), per)] = tot.astype(BF16)

    def get_back(i, c):
        s = lax.rem(base + span + i, n_fs)
        spot = pl.ds(pl.multiple_of(s * quarter, quarter), quarter)
        remote(final.at[spot], final.at[spot], fr_sem.at[s], fr_sem.at[s], {"fs": s}).wait_recv()
        return c

    lax.fori_loop(0, n_fs - span, get_back, 0)
    mix_ref[...] = lax.dot_general(
        place, final[...], (((0,), (0,)), ((), ())), preferred_element_type=F32
    ).astype(BF16)

    def drain(i, c):
        j = lax.rem(me + i, n_fs)
        row_copy(j, me).wait_send()
        w_copy(j, me).wait_send()
        for a in range(3):
            z_copy(a, j, me).wait_send()
            y_copy(a, q, j).wait_send()
        return c

    lax.fori_loop(1, n_fs, drain, 0)
    for sg in abroad + (gid,):
        for i in range(1, span):
            part_copy(sg, lax.rem(member + i, span), member).wait_send()
    for sg in abroad:
        for b in range(span):
            back_copy(sg, b, me).wait_send()

    for copy in sent:
        copy.wait_send()


def write_out(*refs):
    half = len(refs) // 2
    ins, outs, sems = refs[:half], refs[half : 2 * half], refs[2 * half]
    copies = [pltpu.make_async_copy(a, b, sems.at[i]) for i, (a, b) in enumerate(zip(ins, outs))]
    for copy in copies:
        copy.start()
    for copy in copies:
        copy.wait()


def solution(mesh):
    n_fs, n_tp = mesh.shape["fs"], mesh.shape["tp"]

    def on_device(tokens, route_ids, route_weights, ffn_gain, gate_master, up_master, down_master):
        toks, d = tokens.shape
        experts, rows, width = gate_master.shape
        down_rows, cols = down_master.shape[1:]
        served = experts // n_fs
        span = GROUP_SIZE // served
        per = toks // (experts // GROUP_SIZE)
        all_rows = n_fs * per
        quarter = per // span
        dma = pltpu.SemaphoreType.DMA
        shape = jax.ShapeDtypeStruct
        vmem, hbm = pl.BlockSpec(memory_space=pltpu.VMEM), pl.BlockSpec(memory_space=pl.ANY)
        groups = n_fs // span
        out_shape = (
            shape((served, n_fs * rows, width), BF16),
            shape((served, n_fs * rows, width), BF16),
            shape((served, n_fs * down_rows, cols), BF16),
            shape((toks, cols), BF16),
        )
        results = pl.pallas_call(
            functools.partial(kernel, n_fs, n_tp, span),
            out_shape=out_shape,
            in_specs=[hbm] * 7,
            out_specs=(vmem,) * 4,
            scratch_shapes=[
                pltpu.VMEM((toks, d), BF16),
                pltpu.VMEM((2, toks), jnp.int32),
                pltpu.VMEM((2, toks), F32),
                pltpu.VMEM((1, rows), F32),
                pltpu.VMEM((span, per, cols), BF16),
                pltpu.VMEM((span, per, cols), BF16),
                pltpu.VMEM((n_fs, rows, width), F32),
                pltpu.VMEM((n_fs, rows, width), F32),
                pltpu.VMEM((n_fs, down_rows, cols), F32),
                pltpu.VMEM((rows, width), F32),
                pltpu.VMEM((rows, width), F32),
                pltpu.VMEM((down_rows, cols), F32),
                pltpu.VMEM((n_fs, rows, width), BF16),
                pltpu.VMEM((n_fs, rows, width), BF16),
                pltpu.VMEM((n_fs, down_rows, cols), BF16),
                pltpu.VMEM((toks, cols), BF16),
                pltpu.VMEM((n_fs, served, 128), F32),
                pltpu.VMEM((n_tp, 2, all_rows // 2, cols), BF16),
                pltpu.VMEM((n_fs, served, 128), F32),
                pltpu.VMEM((n_tp, served, all_rows // 2, width), BF16),
                pltpu.VMEM((served, all_rows, 128), F32),
                pltpu.VMEM((n_fs * served, per // 2, 128), BF16),
                pltpu.VMEM((n_fs * served, per, 128), BF16),
                pltpu.VMEM((groups, span, span * quarter, cols), BF16),
                pltpu.VMEM((groups, span, span * quarter, cols), BF16),
                pltpu.VMEM((groups, span * quarter, cols), BF16),
                pltpu.VMEM((n_fs * quarter, cols), BF16),
                dma((10,)),
                dma((3, n_fs)),
                dma((3, n_fs)),
                dma((3, n_fs)),
                dma((3, n_fs)),
                dma((2, n_fs)),
                dma((n_fs,)),
                dma((n_fs,)),
                dma((8,)),
                dma((8,)),
                dma((8,)),
                dma((8,)),
                dma((groups, span)),
                dma((groups, span)),
                dma((groups, span)),
                dma((n_fs,)),
            ],
            compiler_params=pltpu.CompilerParams(
                collective_id=0, has_side_effects=True, vmem_limit_bytes=50 * 1024 * 1024
            ),
            name="experts",
        )(
            tokens,
            route_ids.T,
            route_weights.T,
            ffn_gain.reshape(1, rows),
            gate_master.reshape(n_fs, served, rows, width),
            up_master.reshape(n_fs, served, rows, width),
            down_master.reshape(n_fs, served, down_rows, cols),
        )
        return tuple(
            pl.pallas_call(
                write_out,
                out_shape=out_shape,
                in_specs=[vmem] * 4,
                out_specs=(hbm,) * 4,
                scratch_shapes=[dma((4,))],
                compiler_params=pltpu.CompilerParams(vmem_limit_bytes=8 * 1024 * 1024),
                name="write_out",
            )(*results)
        )

    in_specs = (
        P(("grp", "fs"), None),
        P(("grp", "fs"), None),
        P(("grp", "fs"), None),
        P("fs"),
        P(None, "fs", "tp"),
        P(None, "fs", "tp"),
        P(None, "fs", "tp"),
    )
    out_specs = (
        P(("grp", "fs"), None, "tp"),
        P(("grp", "fs"), None, "tp"),
        P(("grp", "fs"), None, "tp"),
        P(("grp", "fs"), "tp"),
    )
    return jax.shard_map(
        on_device, mesh=mesh, in_specs=in_specs, out_specs=out_specs, check_vma=False
    )
```

```python
import functools

import jax
import jax.numpy as jnp
from jax import lax
from jax.experimental import pallas as pl
from jax.experimental.pallas import tpu as pltpu
from jax.sharding import PartitionSpec as P

GROUP_SIZE = 8
MESH = pl.DeviceIdType.MESH
BF16 = jnp.bfloat16
F32 = jnp.float32
PASS_GATE_UP = (6, 8)
PASS_DOWN = (5, 9)


def remote(src, dst, send, recv, where):
    return pltpu.make_async_remote_copy(
        src_ref=src, dst_ref=dst, send_sem=send, recv_sem=recv, device_id=where, device_id_type=MESH
    )


def kernel(
    n_fs, n_tp, span,
    tok_hbm, small_hbm, gm_ref, um_ref, dm_ref,
    og, ou, od, mix_ref,
    tok_ref, small_ref, own_part, own_in,
    g_in, u_in, d_in, g_own, u_own, d_own, g_send, u_send, d_send,
    s_buf, w_send, x_buf, w_recv, h_buf, w_rows, pick, spread, part, gathered, total, final,
    load_sem, z_send, z_recv, y_send, y_recv, w_sems, t_send, t_recv,
    xs_sem, xr_sem, hs_sem, hr_sem, ps_sem, pr_sem, fs_sem, fr_sem,
):
    grp, me, t = lax.axis_index("grp"), lax.axis_index("fs"), lax.axis_index("tp")
    q = lax.rem(grp, 2)
    other = 1 - q
    mate = grp + 1 - 2 * q
    right, left = lax.rem(t + 2, n_tp), lax.rem(t + n_tp - 2, n_tp)
    far = lax.rem(t + 4, n_tp)
    twin = t + 1 - 2 * lax.rem(t, 2)
    member = lax.rem(me, span)
    base = me - member
    groups = n_fs // span
    gid = lax.div(me, span)
    gnext, gprev, gopp = (lax.rem(gid + k, groups) for k in (1, groups - 1, groups // 2))
    toks = tok_ref.shape[0]
    cols = s_buf.shape[1]
    per = s_buf.shape[0] // groups
    quarter = per // span
    slots = per // 2

    def turn(i):
        half = lax.div(i, 2)
        odd = lax.rem(i, 2)
        return half + 1 + odd * (n_fs - 2 * half - 2)

    barrier = pltpu.get_barrier_semaphore()

    def greet(i, c):
        pl.semaphore_signal(
            barrier, inc=1, device_id={"fs": lax.rem(me + i, n_fs)}, device_id_type=MESH
        )
        return c

    lax.fori_loop(1, n_fs, greet, 0)
    pl.semaphore_signal(barrier, inc=1, device_id={"grp": mate}, device_id_type=MESH)
    for peer in (right, left, twin):
        pl.semaphore_signal(barrier, inc=1, device_id={"tp": peer}, device_id_type=MESH)

    loads = [
        pltpu.make_async_copy(gm_ref.at[:, q], g_in, load_sem.at[0]),
        pltpu.make_async_copy(um_ref.at[:, q], u_in, load_sem.at[1]),
        pltpu.make_async_copy(dm_ref.at[:, q], d_in, load_sem.at[2]),
        pltpu.make_async_copy(gm_ref.at[me, other], g_own, load_sem.at[3]),
        pltpu.make_async_copy(um_ref.at[me, other], u_own, load_sem.at[4]),
        pltpu.make_async_copy(dm_ref.at[me, other], d_own, load_sem.at[5]),
    ]
    small = [
        pltpu.make_async_copy(a, b, load_sem.at[6 + i])
        for i, (a, b) in enumerate(
            ((small_hbm, small_ref), (tok_hbm, tok_ref))
        )
    ]
    for load in small + loads:
        load.start()

    for load in small:
        load.wait()
    first, second = small_ref[0:1], small_ref[1:2]
    group = jnp.floor(first * (1.0 / GROUP_SIZE))
    group_hot = (group == lax.broadcasted_iota(jnp.int32, (8, toks), 0).astype(F32)).astype(F32)
    row = lax.broadcasted_iota(jnp.int32, (toks, toks), 0)
    col = lax.broadcasted_iota(jnp.int32, (toks, toks), 1)
    counts = jnp.dot(
        group_hot.astype(BF16), (row < col).astype(BF16), preferred_element_type=F32
    )
    rank = jnp.sum(counts * group_hot, axis=0, keepdims=True)
    target = group * per + rank
    place = (target == row.astype(F32)).astype(BF16)
    tok = tok_ref[...].astype(F32)
    scale = lax.rsqrt(jnp.mean(tok * tok, axis=1, keepdims=True) + 1e-06)
    own = tok_ref[:, pl.ds(pl.multiple_of(t * cols, cols), cols)].astype(F32)
    normed = (own * scale).astype(BF16)
    s_buf[...] = jnp.dot(place, normed, preferred_element_type=F32).astype(BF16)
    rw = small_ref[2:4]
    expert = lax.broadcasted_iota(jnp.int32, (2 * n_fs, toks), 0).astype(F32)
    by_expert = jnp.where(first == expert, rw[0:1], 0.0) + jnp.where(second == expert, rw[1:2], 0.0)
    rank_hot = (rank == lax.broadcasted_iota(jnp.int32, (128, toks), 0).astype(F32)).astype(F32)
    w_all = lax.dot_general(
        by_expert, rank_hot, (((1,), (1,)), ((), ())),
        preferred_element_type=F32, precision=lax.Precision.HIGHEST,
    )
    for j in range(n_fs):
        w_send[j] = w_all[2 * j : 2 * j + 2]

    pl.semaphore_wait(barrier, n_fs - 1 + 4)

    x_half = x_buf.shape[2] // per

    def rows_at(s):
        return x_buf.at[
            t, lax.div(s, x_half), pl.ds(pl.multiple_of(lax.rem(s, x_half) * per, per), per)
        ]

    def row_copy(j, s):
        begin = pl.multiple_of(lax.div(j, span) * per, per)
        return remote(
            s_buf.at[pl.ds(begin, per)], rows_at(s), t_send.at[j], t_recv.at[s], {"fs": j}
        )

    def w_copy(j, s):
        return remote(w_send.at[j], w_recv.at[s], w_sems.at[0, j], w_sems.at[1, s], {"fs": j})

    def dispatch(i, c):
        j = lax.rem(me + turn(i), n_fs)
        row_copy(j, me).start()
        w_copy(j, me).start()
        return c

    lax.fori_loop(0, n_fs - 1, dispatch, 0)

    gain_row = small_ref[4:5, : g_own.shape[0]]
    side = gain_row.shape[1]
    diagonal = lax.broadcasted_iota(jnp.int32, (side, side), 0) == lax.broadcasted_iota(
        jnp.int32, (side, side), 1
    )
    gain = jnp.broadcast_to(
        jnp.sum(jnp.where(diagonal, gain_row, 0.0), axis=1, keepdims=True), g_own.shape
    )
    gate_rows, down_rows = g_own.shape[0], d_own.shape[0]

    def gate_at(buf, e, s):
        return buf.at[e, pl.ds(pl.multiple_of(s * gate_rows, gate_rows), gate_rows)]

    def down_at(buf, e, s):
        return buf.at[e, pl.ds(pl.multiple_of(s * down_rows, down_rows), down_rows)]

    def z_copy(a, j, s):
        src = (g_send, u_send, d_send)[a].at[j]
        dst = (gate_at(og, q, s), gate_at(ou, q, s), down_at(od, q, s))[a]
        return remote(src, dst, z_send.at[a, j], z_recv.at[a, s], {"fs": j})

    def y_copy(a, e, s):
        spot = (gate_at(og, e, s), gate_at(ou, e, s), down_at(od, e, s))[a]
        return remote(spot, spot, y_send.at[a, s], y_recv.at[a, s], {"grp": mate})

    def send_gate_up(i, c):
        j = lax.rem(me + turn(i), n_fs)
        g_send[j] = (g_in[j] * gain).astype(BF16)
        u_send[j] = (u_in[j] * gain).astype(BF16)
        z_copy(0, j, me).start()
        z_copy(1, j, me).start()
        return c

    def send_down(i, c):
        j = lax.rem(me + turn(i), n_fs)
        d_send[j] = d_in[j].astype(BF16)
        z_copy(2, j, me).start()
        return c

    def pass_on(arrays, begin, end):
        def one(i, c):
            s = lax.rem(me + n_fs - turn(i), n_fs)
            for a in arrays:
                z_copy(a, s, s).wait_recv()
                y_copy(a, q, s).start()
            return c

        lax.fori_loop(begin, end, one, 0)

    def from_mate(arrays):
        def one(i, c):
            s = lax.rem(me + n_fs - turn(i), n_fs)
            for a in arrays:
                y_copy(a, other, s).wait_recv()
            return c

        lax.fori_loop(0, n_fs - 1, one, 0)

    last = n_fs - 1
    loads[0].wait()
    loads[1].wait()
    lax.fori_loop(0, last, send_gate_up, 0)
    for load in loads[2:]:
        load.wait()
    lax.fori_loop(0, last, send_down, 0)
    own_rows = s_buf[pl.ds(pl.multiple_of(gid * per, per), per)]
    x_buf[t, lax.div(me, x_half), pl.ds(pl.multiple_of(lax.rem(me, x_half) * per, per), per)] = own_rows
    w_recv[me] = w_send[me]

    def tp_gather(buf, send, recv, between):
        def to(block, k, peer):
            return remote(block, block, send.at[k], recv.at[k], {"tp": peer})

        one = [to(buf.at[t], 0, right), to(buf.at[t], 1, left), to(buf.at[t], 4, twin)]
        for copy in one:
            copy.start()
        between[0]()
        to(buf.at[left], 0, right).wait_recv()
        two = [to(buf.at[left, 0], 2, right), to(buf.at[left], 5, twin)]
        for copy in two:
            copy.start()
        to(buf.at[right], 1, left).wait_recv()
        three = [to(buf.at[right, 1], 3, left), to(buf.at[right], 6, twin)]
        for copy in three:
            copy.start()
        between[1]()
        to(buf.at[far, 0], 2, right).wait_recv()
        to(buf.at[far, 1], 3, left).wait_recv()
        four = [to(buf.at[far], 7, twin)]
        four[0].start()
        between[2]()
        for k, shift in ((4, 0), (5, n_tp - 2), (6, 2), (7, 4)):
            to(buf.at[lax.rem(twin + shift, n_tp)], k, twin).wait_recv()
        return one + two + three + four

    eye = (
        lax.broadcasted_iota(jnp.int32, (per, 128), 0) == lax.broadcasted_iota(jnp.int32, (per, 128), 1)
    ).astype(F32)
    before = (
        lax.broadcasted_iota(jnp.int32, (128, 128), 0) < lax.broadcasted_iota(jnp.int32, (128, 128), 1)
    ).astype(BF16)
    slot_down = lax.broadcasted_iota(jnp.int32, (slots, 128), 0).astype(F32)
    slot_along = lax.broadcasted_iota(jnp.int32, (per, 128), 1).astype(F32)

    def index_rows():
        def one(s, c):
            both = w_recv[s]
            used = both > 0.0
            at = jnp.dot(used.astype(BF16), before, preferred_element_type=F32)
            at = jnp.where(used, at, -1.0)
            for k in range(2):
                pick[2 * s + k] = (at[k : k + 1] == slot_down).astype(BF16)
                column = jnp.sum(eye * both[k : k + 1], axis=1, keepdims=True)
                w_rows[k, pl.ds(pl.multiple_of(s * per, per), per)] = jnp.broadcast_to(column, (per, 128))
                at_col = jnp.sum(eye * at[k : k + 1], axis=1, keepdims=True)
                spread[2 * s + k] = (at_col == slot_along).astype(BF16)
            return c

        lax.fori_loop(0, n_fs, one, 0)

    def own_blocks():
        gate_spot = pl.ds(pl.multiple_of(me * gate_rows, gate_rows), gate_rows)
        down_spot = pl.ds(pl.multiple_of(me * down_rows, down_rows), down_rows)
        og[q, gate_spot] = (g_in[me] * gain).astype(BF16)
        ou[q, gate_spot] = (u_in[me] * gain).astype(BF16)
        od[q, down_spot] = d_in[me].astype(BF16)
        og[other, gate_spot] = (g_own[...] * gain).astype(BF16)
        ou[other, gate_spot] = (u_own[...] * gain).astype(BF16)
        od[other, down_spot] = d_own[...].astype(BF16)

    def rows_in(i, c):
        s = lax.rem(me + n_fs - turn(i), n_fs)
        row_copy(s, s).wait_recv()
        w_copy(s, s).wait_recv()
        return c

    own_blocks()
    lax.fori_loop(0, last, rows_in, 0)

    def while_x():
        index_rows()
        pass_on((0, 1), 0, PASS_GATE_UP[0])

    sent = tp_gather(
        x_buf, xs_sem, xr_sem,
        (
            while_x,
            lambda: pass_on((0, 1), PASS_GATE_UP[0], PASS_GATE_UP[1]),
            lambda: pass_on((0, 1), PASS_GATE_UP[1], last),
        ),
    )
    from_mate((0, 1))

    width = og.shape[2]
    tile = x_buf.shape[2]

    def hidden(i, c):
        half, k = lax.div(i, 2), lax.rem(i, 2)
        acc = jnp.zeros((tile, 2 * width), F32)
        for f in range(n_tp):
            w = jnp.concatenate(
                [og[k, f * cols : (f + 1) * cols], ou[k, f * cols : (f + 1) * cols]], axis=1
            )
            acc += jnp.dot(x_buf[f, half], w, preferred_element_type=F32)
        g, u = acc[:, :width], acc[:, width:]
        act = (g / (1.0 + jnp.exp(-g)) * u).astype(BF16)
        for b in range(tile // per):
            s = half * x_half + b
            rows = jnp.dot(
                pick[2 * s + k][:, :per], act[b * per : (b + 1) * per], preferred_element_type=F32
            )
            h_buf[t, k, pl.ds(pl.multiple_of(s * slots, slots), slots)] = rows.astype(BF16)
        return c

    lax.fori_loop(0, 4, hidden, 0)
    sent += tp_gather(
        h_buf, hs_sem, hr_sem,
        (
            lambda: pass_on((2,), 0, PASS_DOWN[0]),
            lambda: pass_on((2,), PASS_DOWN[0], PASS_DOWN[1]),
            lambda: pass_on((2,), PASS_DOWN[1], last),
        ),
    )
    from_mate((2,))

    deep = span * slots

    def outputs(sg):
        rows = pl.ds(pl.multiple_of(sg * deep, deep), deep)
        outs = []
        for k in range(2):
            acc = jnp.zeros((deep, cols), F32)
            for f in range(n_tp // 2):
                h = jnp.concatenate([h_buf[2 * f, k, rows], h_buf[2 * f + 1, k, rows]], axis=1)
                acc += jnp.dot(
                    h, od[k, 2 * f * width : 2 * (f + 1) * width], preferred_element_type=F32
                )
            outs.append(acc.astype(BF16))
        for b in range(span):
            s = sg * span + b
            mix = jnp.zeros((per, cols), F32)
            for k in range(2):
                full = jnp.dot(
                    spread[2 * s + k][:, :slots], outs[k][b * slots : (b + 1) * slots],
                    preferred_element_type=F32,
                )
                w = w_rows[k, pl.ds(pl.multiple_of(s * per, per), per)]
                mix += full * jnp.concatenate([w] * (cols // 128), axis=1)
            mix = mix.astype(BF16)
            if sg is gid:
                own_part[b] = mix
                continue
            for m in range(span):
                part[sg, m, b * quarter : (b + 1) * quarter] = mix[m * quarter : (m + 1) * quarter]

    def part_copy(sg, to_member, from_member):
        direct = sg is gid
        return remote(
            own_part.at[to_member] if direct else part.at[sg, to_member],
            own_in.at[from_member] if direct else gathered.at[sg, from_member],
            ps_sem.at[sg, to_member], pr_sem.at[sg, from_member], {"fs": base + to_member},
        )

    def back_copy(sg, b, s):
        return remote(
            total.at[sg, b * quarter : (b + 1) * quarter],
            final.at[pl.ds(pl.multiple_of(s * quarter, quarter), quarter)],
            fs_sem.at[sg, b], fr_sem.at[s], {"fs": sg * span + b},
        )

    abroad = (gopp, gnext, gprev)
    for sg in abroad:
        outputs(sg)
        for i in range(1, span):
            part_copy(sg, lax.rem(member + i, span), member).start()
    outputs(gid)
    for sg in abroad:
        tot = part[sg, member].astype(F32)
        for i in range(1, span):
            frm = lax.rem(member + span - i, span)
            part_copy(sg, frm, frm).wait_recv()
            tot += gathered[sg, frm].astype(F32)
        total[sg] = tot.astype(BF16)
        for b in range(span):
            back_copy(sg, b, me).start()
        if sg is gopp:
            for i in range(1, span):
                part_copy(gid, lax.rem(member + i, span), member).start()

    tot = own_part[member].astype(F32)
    for i in range(1, span):
        frm = lax.rem(member + span - i, span)
        part_copy(gid, frm, frm).wait_recv()
        tot += own_in[frm].astype(F32)
    final[pl.ds(pl.multiple_of(gid * per, per), per)] = tot.astype(BF16)

    def get_back(i, c):
        s = lax.rem(base + span + i, n_fs)
        spot = pl.ds(pl.multiple_of(s * quarter, quarter), quarter)
        remote(final.at[spot], final.at[spot], fr_sem.at[s], fr_sem.at[s], {"fs": s}).wait_recv()
        return c

    lax.fori_loop(0, n_fs - span, get_back, 0)
    mix_ref[...] = lax.dot_general(
        place, final[...], (((0,), (0,)), ((), ())), preferred_element_type=F32
    ).astype(BF16)

    def drain(i, c):
        j = lax.rem(me + i, n_fs)
        row_copy(j, me).wait_send()
        w_copy(j, me).wait_send()
        for a in range(3):
            z_copy(a, j, me).wait_send()
            y_copy(a, q, j).wait_send()
        return c

    lax.fori_loop(1, n_fs, drain, 0)
    for sg in abroad + (gid,):
        for i in range(1, span):
            part_copy(sg, lax.rem(member + i, span), member).wait_send()
    for sg in abroad:
        for b in range(span):
            back_copy(sg, b, me).wait_send()

    for copy in sent:
        copy.wait_send()


def write_out(*refs):
    half = len(refs) // 2
    ins, outs, sems = refs[:half], refs[half : 2 * half], refs[2 * half]
    copies = [pltpu.make_async_copy(a, b, sems.at[i]) for i, (a, b) in enumerate(zip(ins, outs))]
    for copy in copies:
        copy.start()
    for copy in copies:
        copy.wait()


def solution(mesh):
    n_fs, n_tp = mesh.shape["fs"], mesh.shape["tp"]

    def on_device(tokens, route_ids, route_weights, ffn_gain, gate_master, up_master, down_master):
        toks, d = tokens.shape
        experts, rows, width = gate_master.shape
        down_rows, cols = down_master.shape[1:]
        served = experts // n_fs
        span = GROUP_SIZE // served
        per = toks // (experts // GROUP_SIZE)
        all_rows = n_fs * per
        quarter = per // span
        dma = pltpu.SemaphoreType.DMA
        shape = jax.ShapeDtypeStruct
        vmem, hbm = pl.BlockSpec(memory_space=pltpu.VMEM), pl.BlockSpec(memory_space=pl.ANY)
        groups = n_fs // span
        out_shape = (
            shape((served, n_fs * rows, width), BF16),
            shape((served, n_fs * rows, width), BF16),
            shape((served, n_fs * down_rows, cols), BF16),
            shape((toks, cols), BF16),
        )
        small = (
            jnp.pad(route_ids.T.astype(F32), ((0, 6), (0, 0)))
            + jnp.pad(route_weights.T, ((2, 4), (0, 0)))
            + jnp.pad(ffn_gain.reshape(1, rows), ((4, 3), (0, toks - rows)))
        )
        results = pl.pallas_call(
            functools.partial(kernel, n_fs, n_tp, span),
            out_shape=out_shape,
            in_specs=[hbm] * 5,
            out_specs=(vmem,) * 4,
            scratch_shapes=[
                pltpu.VMEM((toks, d), BF16),
                pltpu.VMEM((8, toks), F32),
                pltpu.VMEM((span, per, cols), BF16),
                pltpu.VMEM((span, per, cols), BF16),
                pltpu.VMEM((n_fs, rows, width), F32),
                pltpu.VMEM((n_fs, rows, width), F32),
                pltpu.VMEM((n_fs, down_rows, cols), F32),
                pltpu.VMEM((rows, width), F32),
                pltpu.VMEM((rows, width), F32),
                pltpu.VMEM((down_rows, cols), F32),
                pltpu.VMEM((n_fs, rows, width), BF16),
                pltpu.VMEM((n_fs, rows, width), BF16),
                pltpu.VMEM((n_fs, down_rows, cols), BF16),
                pltpu.VMEM((toks, cols), BF16),
                pltpu.VMEM((n_fs, served, 128), F32),
                pltpu.VMEM((n_tp, 2, all_rows // 2, cols), BF16),
                pltpu.VMEM((n_fs, served, 128), F32),
                pltpu.VMEM((n_tp, served, all_rows // 2, width), BF16),
                pltpu.VMEM((served, all_rows, 128), F32),
                pltpu.VMEM((n_fs * served, per // 2, 128), BF16),
                pltpu.VMEM((n_fs * served, per, 128), BF16),
                pltpu.VMEM((groups, span, span * quarter, cols), BF16),
                pltpu.VMEM((groups, span, span * quarter, cols), BF16),
                pltpu.VMEM((groups, span * quarter, cols), BF16),
                pltpu.VMEM((n_fs * quarter, cols), BF16),
                dma((8,)),
                dma((3, n_fs)),
                dma((3, n_fs)),
                dma((3, n_fs)),
                dma((3, n_fs)),
                dma((2, n_fs)),
                dma((n_fs,)),
                dma((n_fs,)),
                dma((8,)),
                dma((8,)),
                dma((8,)),
                dma((8,)),
                dma((groups, span)),
                dma((groups, span)),
                dma((groups, span)),
                dma((n_fs,)),
            ],
            compiler_params=pltpu.CompilerParams(
                collective_id=0, has_side_effects=True, vmem_limit_bytes=50 * 1024 * 1024
            ),
            name="experts",
        )(
            tokens,
            small,
            gate_master.reshape(n_fs, served, rows, width),
            up_master.reshape(n_fs, served, rows, width),
            down_master.reshape(n_fs, served, down_rows, cols),
        )
        return tuple(
            pl.pallas_call(
                write_out,
                out_shape=out_shape,
                in_specs=[vmem] * 4,
                out_specs=(hbm,) * 4,
                scratch_shapes=[dma((4,))],
                compiler_params=pltpu.CompilerParams(vmem_limit_bytes=8 * 1024 * 1024),
                name="write_out",
            )(*results)
        )

    in_specs = (
        P(("grp", "fs"), None),
        P(("grp", "fs"), None),
        P(("grp", "fs"), None),
        P("fs"),
        P(None, "fs", "tp"),
        P(None, "fs", "tp"),
        P(None, "fs", "tp"),
    )
    out_specs = (
        P(("grp", "fs"), None, "tp"),
        P(("grp", "fs"), None, "tp"),
        P(("grp", "fs"), None, "tp"),
        P(("grp", "fs"), "tp"),
    )
    return jax.shard_map(
        on_device, mesh=mesh, in_specs=in_specs, out_specs=out_specs, check_vma=False
    )
```
